768 devices in a mesh: ep: 24 (over z, core), tp: 32 (over y, x).
Axes of the slice: x: 4, y: 8, z: 12, core: 2. Of those that a mesh axis runs over, the one named last changes fastest.
Arguments:
- tokens: bfloat16 [768, 4096], P('ep'), may hold values from -6 to 6
- norm_gains: float32 [4, 4096], replicated, may hold values from 0.1 to 1.9
- w_query: bfloat16 [4096, 4096], P(None, 'tp'), may hold values from -0.09375 to 0.09375
- w_query_rope: bfloat16 [4096, 2048], P(None, 'tp'), may hold values from -0.09375 to 0.09375
- w_key_up: bfloat16 [32, 128, 1024], P('tp'), may hold values from -0.5 to 0.5
- w_value_up: bfloat16 [32, 1024, 128], P('tp'), may hold values from -0.1875 to 0.1875
- w_output: bfloat16 [4096, 4096], P('tp'), may hold values from -0.09375 to 0.09375
- w_latent_down: bfloat16 [4096, 1024], P(None, 'tp'), may hold values from -0.09375 to 0.09375
- latent_gain: float32 [1024], replicated, may hold values from 0.1 to 1.9
- w_rope_down: bfloat16 [4096, 64], replicated, may hold values from -0.09375 to 0.09375
- cache_latent: bfloat16 [768, 1024, 1024], P(('ep', 'tp')), may hold values from -300 to 300
- cache_rope: bfloat16 [768, 1024, 64], P(('ep', 'tp')), may hold values from -6 to 6
- lengths: int32 [768], P(('ep', 'tp')), may hold values from 1 to 1024, as said below
- routes: int32 [768, 2], P('ep'), may hold values from 0 to 23, all different within a row; in each aligned block of 32 rows (0 to 31, 32 to 63, ...) at most 5 rows name the same one
- route_weights: float32 [768, 2], P('ep'), may hold values from 0.2 to 1
- w_gate: bfloat16 [24, 4096, 2048], P('ep', None, 'tp'), may hold values from -0.09375 to 0.09375
- w_up: bfloat16 [24, 4096, 2048], P('ep', None, 'tp'), may hold values from -0.09375 to 0.09375
- w_down: bfloat16 [24, 2048, 4096], P('ep', 'tp'), may hold values from -0.125 to 0.125
Outputs:
- hidden_out: bfloat16 [768, 4096], P(('ep', 'tp'))
- new_latent: bfloat16 [768, 1024], P(('ep', 'tp'))
- new_rope: bfloat16 [768, 64], P(('ep', 'tp'))
The draws below stay inside these ranges and needn't reach their ends.
Inputs may be any that keep to these rules, and one draw needn't show every extreme that they name: `routes`: within each aligned block of 32 rows no expert is named by more than 5 rows, a bound that some block reaches; the 2 experts of a row differ. The new token stands at position lengths; some sequence has exactly 1024.
All inputs are finite; a program needn't handle non-finite values.
Results may differ from the reference program's by a relative error of at most 0.02.
Values may be sent and summed in bfloat16 or wider, within the bound.
A program may use at most 32 MiB of HBM per device.

```python
import math
import jax
import jax.numpy as jnp
import numpy as np
from jax import lax

D = 4096
HEADS = 32
NOPE = 128
ROPE = 64
VDIM = 128
LATENT = 1024
FF = 2048
TOPK = 2
EXP_LOCAL = 1
CACHE = 1024
EXPERTS = 24
GROUP_ROWS = 32
TOKENS = 768
CAP = 5
FF_DEV = 64
N_EP = 24


def draw_cache_latent(key, part):
    base_key = jax.random.fold_in(jax.random.fold_in(key, 11), 0)
    drawn = jnp.clip(jax.random.normal(base_key, (TOKENS, CACHE, LATENT), jnp.float32), -6.0, 6.0)
    return drawn.astype(jnp.bfloat16)


def draw_lengths(key, part):
    value_key, place_key = jax.random.split(jax.random.fold_in(key, 13))
    drawn = jax.random.randint(value_key, (TOKENS,), 1, CACHE + 1)
    longest = jax.random.randint(place_key, (), 0, TOKENS)
    return jnp.where(jnp.arange(TOKENS) == longest, CACHE, drawn).astype(jnp.int32)


def block_levels(key, extent, cuts, least, high):
    gain = 1.0
    for dim, blocks in cuts:
        steps = jax.random.uniform(jax.random.fold_in(jax.random.fold_in(key, 6), dim), (blocks,), jnp.float32, least / len(cuts), high / len(cuts))
        gain = gain * jnp.repeat(jnp.exp(steps), extent[dim] // blocks).reshape((-1,) + (1,) * (len(extent) - 1 - dim))
    return gain


def shared_out(stream_key, own, number, rows, count, top, reach, lean):
    sequence = jax.random.permutation(stream_key, count)
    crowded, ordinary = load_shares(count, rows * top, reach, lean, True), load_shares(count, rows * top, reach, lean, False)
    places = jnp.arange(count)

    def named(sizes, rotation):
        used = int((sizes > 0).sum())
        fixed = max(1, used // 4)
        shifted = fixed + (places - fixed + rotation * (used - fixed)) % max(1, count - fixed)
        return jnp.zeros((count,), jnp.int32).at[sequence[jnp.where(places < fixed, places, shifted)]].set(jnp.asarray(sizes, jnp.int32))

    sizes = jnp.where(number % 4 == 0, named(crowded, number // 4), named(ordinary, number - number // 4 - 1))
    mixed = jax.random.permutation(jax.random.fold_in(own, 3), count)
    source_of, receiver = mixed[0:count // 2 * 2:2], mixed[1:count // 2 * 2:2]
    slack = jnp.minimum(sizes[source_of] - 1, reach - sizes[receiver]) // 2
    slack = jnp.where((source_of == sequence[0]) | (receiver == sequence[0]) | (sizes[receiver] == 0), 0, jnp.maximum(slack, 0))
    shifted = jax.random.randint(jax.random.fold_in(own, 4), (count // 2,), 0, 1 << 20) % (slack + 1)
    sizes = sizes.at[source_of].add(-shifted).at[receiver].add(shifted)
    items = jnp.searchsorted(jnp.cumsum(sizes), jnp.arange(rows * top), side="right").astype(jnp.int32)
    table = items.reshape(top, rows).T
    table = table[jax.random.permutation(jax.random.fold_in(own, 1), rows)]
    rotation = jax.random.randint(jax.random.fold_in(own, 2), (rows, 1), 0, top)
    return jnp.take_along_axis(table, (jnp.arange(top)[None, :] + rotation) % top, axis=1)


def load_shares(number_of, total, bound, skew, full):
    loads = [(1 << 20) // math.isqrt(grade ** skew) + 1 for grade in range(1, number_of + 1)]
    largest = bound if full else min(bound, max(-(-total // number_of), total * loads[0] // sum(loads)))
    least = 1 if total - largest >= number_of - 1 else 0
    counts, rest = [largest] + [least] * (number_of - 1), total - largest - least * (number_of - 1)
    while rest > 0:
        movable = [i for i in range(1, number_of) if counts[i] < largest] or [i for i in range(1, number_of) if counts[i] < bound]
        mass, remaining = sum([loads[i] for i in movable]), rest
        for i in movable:
            addition = min(bound - counts[i], max(1, remaining * loads[i] // mass), rest)
            counts[i] = counts[i] + addition
            rest = rest - addition
    return np.array(counts)


def normal_values(stream_key, shape, scale, bound, pieces=(), kind=jnp.bfloat16):
    values = jax.random.normal(stream_key, shape, jnp.float32) * scale
    if len(pieces) > 0:
        values = block_levels(stream_key, shape, pieces, -0.22, 0.18) * values
    return jnp.clip(values, min=-bound, max=bound).astype(kind)


def setup_inputs(seed: int = 0) -> dict:
    seeds = jax.random.split(jax.random.key(seed), 19)
    tokens = normal_values(seeds[0], (TOKENS, D), 1.0, 6.0, ((0, 24),))
    norm_gains = jnp.clip(1.0 + 0.18 * jax.random.normal(seeds[1], (4, D), jnp.float32), 0.1, 1.9)
    w_query = normal_values(seeds[2], (D, HEADS * NOPE), D ** -0.5, 0.09375, ((1, 32),))
    w_query_rope = normal_values(seeds[3], (D, HEADS * ROPE), D ** -0.5, 0.09375, ((1, 32),))
    w_key_up = normal_values(seeds[4], (HEADS, NOPE, LATENT), NOPE ** -0.5, 0.5, ((0, 32),))
    w_value_up = normal_values(seeds[5], (HEADS, LATENT, VDIM), LATENT ** -0.5, 0.1875, ((0, 32),))
    w_output = normal_values(seeds[6], (HEADS * VDIM, D), (HEADS * VDIM) ** -0.5, 0.09375, ((0, 32),))
    w_latent_down = normal_values(seeds[7], (D, LATENT), D ** -0.5, 0.09375, ((1, 32),))
    latent_gain = jnp.clip(1.0 + 0.18 * jax.random.normal(seeds[8], (LATENT,), jnp.float32), 0.1, 1.9)
    w_rope_down = normal_values(seeds[9], (D, ROPE), D ** -0.5, 0.09375)
    cache_latent = draw_cache_latent(jax.random.fold_in(seeds[18], 71), 0)
    cache_rope = normal_values(seeds[11], (TOKENS, CACHE, ROPE), 1.0, 6.0, ((0, 768),))
    lengths = draw_lengths(jax.random.fold_in(seeds[18], 71), 0)
    routes_keys = jax.random.split(jax.random.fold_in(seeds[13], 1), TOKENS // GROUP_ROWS)
    routes_turns = jax.random.permutation(jax.random.fold_in(seeds[13], 3), TOKENS // GROUP_ROWS)
    routes = jax.vmap(lambda own, number: shared_out(jax.random.fold_in(seeds[13], 2), own, number, GROUP_ROWS, EXPERTS, TOPK, CAP, 2))(routes_keys, routes_turns).reshape((TOKENS, TOPK))
    route_weights = jnp.clip(0.2 + 0.8 * jax.random.uniform(seeds[14], (TOKENS, TOPK), jnp.float32) ** block_levels(seeds[14], (TOKENS, TOPK), ((0, 24),), -0.2, 0.2), 0.2, 1.0)
    w_gate = normal_values(seeds[15], (EXPERTS // EXP_LOCAL, D, EXP_LOCAL * FF), D ** -0.5, 0.09375, ((0, 24), (2, 32)))
    w_up = normal_values(seeds[16], (EXPERTS // EXP_LOCAL, D, EXP_LOCAL * FF), D ** -0.5, 0.09375, ((0, 24), (2, 32)))
    w_down = normal_values(seeds[17], (EXPERTS // EXP_LOCAL, EXP_LOCAL * FF, D), FF ** -0.5, 0.125, ((0, 24), (1, 32)))
    return dict(tokens=tokens, norm_gains=norm_gains, w_query=w_query, w_query_rope=w_query_rope, w_key_up=w_key_up, w_value_up=w_value_up, w_output=w_output, w_latent_down=w_latent_down, latent_gain=latent_gain, w_rope_down=w_rope_down, cache_latent=cache_latent, cache_rope=cache_rope, lengths=lengths, routes=routes, route_weights=route_weights, w_gate=w_gate, w_up=w_up, w_down=w_down)


EPSILON = 1e-06
ROTARY_BASE = 500000.0

def rms_scale(source, gain_row):
    values_f = source.astype(jnp.float32)
    return values_f * lax.rsqrt(lax.optimization_barrier(jnp.mean(values_f * values_f, axis=-1, keepdims=True)) + EPSILON) * gain_row.astype(jnp.float32)

def rotate(source, position):
    half_width = source.shape[-1] // 2
    frequency = ROTARY_BASE ** (-jnp.arange(half_width, dtype=jnp.float32) / half_width)
    angles = position[..., None] * frequency
    first_half = source[..., :half_width]
    second_half = source[..., half_width:]
    return jnp.concatenate([first_half * jnp.cos(angles) - second_half * jnp.sin(angles), second_half * jnp.cos(angles) + first_half * jnp.sin(angles)], axis=-1)

def attend_one(items):
    q_latent, q_pe, cache_lat, cache_rp, lat_new, rope_new, length = items
    score_scale = (NOPE + ROPE) ** (-0.5)
    scores = (jnp.einsum('hc,pc->hp', q_latent.astype(jnp.float32), cache_lat.astype(jnp.float32)) + jnp.einsum('hr,pr->hp', q_pe.astype(jnp.float32), cache_rp.astype(jnp.float32))) * score_scale
    own_score = (jnp.einsum('hc,c->h', q_latent.astype(jnp.float32), lat_new.astype(jnp.float32)) + jnp.einsum('hr,r->h', q_pe.astype(jnp.float32), rope_new.astype(jnp.float32))) * score_scale
    visible = (jnp.arange(CACHE, dtype=jnp.int32) < length)[None, :]
    row_max = jnp.maximum(lax.optimization_barrier(jnp.max(jnp.where(visible, scores, -jnp.inf), axis=-1)), own_score)
    weights = jnp.where(visible, jnp.exp(scores - row_max[:, None]), 0.0)
    own_weight = jnp.exp(own_score - row_max)
    denominator = lax.optimization_barrier(jnp.sum(weights, axis=-1)) + own_weight
    probabilities = (weights / denominator[:, None]).astype(jnp.bfloat16)
    own_prob = (own_weight / denominator).astype(jnp.bfloat16)
    attended = jnp.einsum('hp,pc->hc', probabilities.astype(jnp.float32), cache_lat.astype(jnp.float32))
    attended = attended + own_prob.astype(jnp.float32)[:, None] * lat_new.astype(jnp.float32)[None, :]
    return attended.astype(jnp.bfloat16)

def expert_total(expert_in, routes, route_weights, w_gate, w_up, w_down):
    slot_count = N_EP * CAP
    block_count = FF // FF_DEV

    def one_expert(running, expert):
        holder = (expert // EXP_LOCAL).astype(jnp.int32)
        offset = (expert % EXP_LOCAL * FF).astype(jnp.int32)
        gate_cols = lax.dynamic_slice_in_dim(w_gate[holder], offset, FF, 1)
        up_cols = lax.dynamic_slice_in_dim(w_up[holder], offset, FF, 1)
        down_rows = lax.dynamic_slice_in_dim(w_down[holder], offset, FF, 0)
        hit_mask = routes == expert
        chosen = jnp.any(hit_mask, axis=-1)
        route_weight = lax.optimization_barrier(jnp.sum(jnp.where(hit_mask, route_weights, 0.0), axis=-1))
        slot_place = (jnp.cumsum(chosen.astype(jnp.int32)) - 1).astype(jnp.int32)
        slot_target = jnp.where(chosen, slot_place, slot_count).astype(jnp.int32)
        row_index = jnp.zeros((slot_count,), jnp.int32).at[slot_target].set(jnp.arange(TOKENS, dtype=jnp.int32), mode='drop')
        expert_rows = expert_in[row_index]
        gate_sum = jnp.dot(expert_rows, gate_cols, preferred_element_type=jnp.float32)
        up_sum = jnp.dot(expert_rows, up_cols, preferred_element_type=jnp.float32)
        hidden_units = (jax.nn.silu(gate_sum) * up_sum).astype(jnp.bfloat16)
        blocks = jnp.einsum('nbf,bfd->nbd', hidden_units.reshape(slot_count, block_count, FF_DEV).astype(jnp.float32), down_rows.reshape(block_count, FF_DEV, D).astype(jnp.float32)).astype(jnp.bfloat16)
        block_sum = lax.optimization_barrier(jnp.sum(blocks.astype(jnp.float32), axis=1))
        picked = block_sum[jnp.clip(slot_place, 0, slot_count - 1).astype(jnp.int32)]
        return (running + jnp.where(chosen[:, None], route_weight[:, None] * picked, 0.0), None)
    start = jnp.zeros((TOKENS, D), jnp.float32)
    return lax.scan(one_expert, start, jnp.arange(EXPERTS, dtype=jnp.int32))[0]

def reference(tokens, norm_gains, w_query, w_query_rope, w_key_up, w_value_up, w_output, w_latent_down, latent_gain, w_rope_down, cache_latent, cache_rope, lengths, routes, route_weights, w_gate, w_up, w_down):
    normed = rms_scale(tokens, norm_gains[0]).astype(jnp.bfloat16)
    q_nope = jnp.dot(normed, w_query, preferred_element_type=jnp.float32).astype(jnp.bfloat16).reshape(TOKENS, HEADS, NOPE)
    q_latent = jnp.einsum('thn,hnc->thc', q_nope.astype(jnp.float32), w_key_up.astype(jnp.float32)).astype(jnp.bfloat16)
    q_rot = jnp.dot(normed, w_query_rope, preferred_element_type=jnp.float32).astype(jnp.bfloat16).reshape(TOKENS, HEADS, ROPE)
    latent_raw = jnp.dot(normed, w_latent_down, preferred_element_type=jnp.float32).astype(jnp.bfloat16)
    rope_raw = jnp.dot(normed, w_rope_down, preferred_element_type=jnp.float32).astype(jnp.bfloat16)
    new_latent = rms_scale(latent_raw, latent_gain).astype(jnp.bfloat16)
    position = lengths.astype(jnp.float32)
    new_rope = rotate(rope_raw.astype(jnp.float32), position).astype(jnp.bfloat16)
    q_pe = rotate(q_rot.astype(jnp.float32), position[:, None]).astype(jnp.bfloat16)
    attended = lax.map(attend_one, (q_latent, q_pe, cache_latent, cache_rope, new_latent, new_rope, lengths))
    values = jnp.einsum('thc,hcv->thv', attended.astype(jnp.float32), w_value_up.astype(jnp.float32)).astype(jnp.bfloat16)
    mixed = jnp.dot(values.reshape(TOKENS, HEADS * VDIM), w_output, preferred_element_type=jnp.float32)
    resid = (tokens.astype(jnp.float32) + rms_scale(mixed, norm_gains[1])).astype(jnp.bfloat16)
    expert_in = rms_scale(resid, norm_gains[2]).astype(jnp.bfloat16)
    routed = expert_total(expert_in, routes, route_weights, w_gate, w_up, w_down)
    hidden_out = (resid.astype(jnp.float32) + rms_scale(routed, norm_gains[3])).astype(jnp.bfloat16)
    return (hidden_out, new_latent, new_rope)
```

```python
import functools
import math

import jax
import jax.numpy as jnp
from jax import lax
from jax.experimental import pallas as pl
from jax.experimental.pallas import tpu as pltpu
from jax.sharding import PartitionSpec as P

EPSILON = 1e-06
ROTARY_BASE = 500000.0
X_SIZE = 4
LANES = 128
CAP = 5
CAP_PAD = 6
BF16 = jnp.bfloat16
F32 = jnp.float32
NT = (((1,), (1,)), ((), ()))


def dot(a, b):
    return jnp.dot(a, b, preferred_element_type=F32)


def dot_nt(a, b):
    return lax.dot_general(a, b, NT, preferred_element_type=F32)


def iota(shape, dim):
    return lax.broadcasted_iota(jnp.int32, shape, dim)


def send_to_all(axis, count, me, source_of, target, send_sem, recv_sem):
    def step(i, carry):
        peer = lax.rem(me + i, count)
        pltpu.make_async_remote_copy(
            src_ref=source_of(peer),
            dst_ref=target,
            send_sem=send_sem,
            recv_sem=recv_sem,
            device_id={axis: peer},
            device_id_type=pl.DeviceIdType.MESH,
        ).start()
        return carry

    lax.fori_loop(1, count, step, 0)


def wait_bytes(ref, sem):
    pltpu.make_async_copy(ref, ref, sem).wait()


def step_kernel(
    n_ep,
    n_tp,
    cap,
    cap_pad,
    score_scale,
    tokens_h,
    gains_h,
    wq_h,
    wqr_h,
    wku_h,
    wvu_h,
    wo_h,
    wld_h,
    lgain_v,
    wrd_h,
    cl_h,
    cr_h,
    len_s,
    routes_v,
    rw_v,
    wg_h,
    wu_h,
    wd_h,
    trig_v,
    out_v,
    nl_v,
    nr_v,
    tok_v,
    gains_v,
    wq_v,
    wside_v,
    wku_v,
    wvu_v,
    wo_v,
    cl_v,
    cr_v,
    wgu_v,
    wd_v,
    load_sem,
    norm_v,
    rows_v,
    scat_v,
    extra1,
    msg1,
    rec1e,
    rec1,
    msg2,
    rec2,
    msg3,
    rec3,
    msg4,
    rec4,
    msg5,
    rec5,
    chunks6,
    msg7,
    rec7,
    msg8,
    rec8,
    msg9,
    rec9,
    pick_v,
    back_v,
    ssem,
    rsem,
    rsem6,
    rsem7,
):
    e = lax.axis_index("ep")
    t = lax.axis_index("tp")
    x = lax.rem(t, X_SIZE)
    y0 = t - x
    rows = tok_v.shape[0]
    nblk = tok_v.shape[1] // LANES
    sub = nblk // X_SIZE
    slots = n_ep * cap_pad
    lat_blk = 8

    loads = [
        (tokens_h, tok_v),
        (gains_h, gains_v),
        (wq_h, wq_v),
        (wqr_h, wside_v.at[0:64]),
        (wrd_h, wside_v.at[64:128]),
        (wld_h, wside_v.at[128 : 128 + wld_h.shape[0]]),
        (wku_h.at[0], wku_v),
        (cl_h.at[0], cl_v),
        (cr_h.at[0], cr_v),
        (wvu_h.at[0], wvu_v),
        (wo_h, wo_v),
        (wg_h.at[0], wgu_v.at[0:64]),
        (wu_h.at[0], wgu_v.at[64:128]),
        (wd_h.at[0], wd_v),
    ]
    copies = [pltpu.make_async_copy(s, d, load_sem.at[i]) for i, (s, d) in enumerate(loads)]
    for c in copies:
        c.start()

    barrier = pltpu.get_barrier_semaphore()

    def greet(axis, count, me):
        def step(i, carry):
            pl.semaphore_signal(
                barrier,
                inc=1,
                device_id={axis: lax.rem(me + i, count)},
                device_id_type=pl.DeviceIdType.MESH,
            )
            return carry

        lax.fori_loop(1, count, step, 0)

    greet("tp", n_tp, t)
    greet("ep", n_ep, e)

    copies[0].wait()
    copies[1].wait()
    tok = tok_v[...].astype(F32)
    scale0 = lax.rsqrt(jnp.mean(tok * tok, axis=-1, keepdims=True) + EPSILON)
    norm_v[...] = (tok * scale0 * gains_v[0:1, :]).astype(BF16)
    copies[2].wait()
    q_nope = dot(norm_v[...], wq_v[...]).astype(BF16)
    copies[6].wait()
    q_lat = dot(q_nope, wku_v[...])
    for j in range(lat_blk):
        scat_v[j * rows : (j + 1) * rows, :] = q_lat[:, j * LANES : (j + 1) * LANES]
    for r in range(rows):
        msg1[r] = scat_v[pl.ds(r, lat_blk, stride=rows), :].astype(BF16)
    for i in (3, 4, 5):
        copies[i].wait()
    side = dot_nt(norm_v[...], wside_v[...]).astype(BF16)
    q_rot = side[:, 0:64]
    rope_all = side[:, 64:128].astype(F32)
    cols = wld_h.shape[0]
    per_row = LANES // cols
    lat_cols = side[:, 128 : 128 + cols]
    place = (iota((cols, LANES), 1) == iota((cols, LANES), 0) + cols * lax.rem(t, per_row)).astype(F32).astype(BF16)
    widen = (iota((64, LANES), 1) == iota((64, LANES), 0)).astype(F32).astype(BF16)
    extra1[:, 0, 0:LANES] = dot(q_rot, widen)
    extra1[:, 0, LANES : 2 * LANES] = dot(lat_cols, place)
    rec1[t] = msg1[t]
    rec1e[t] = extra1[t]

    pl.semaphore_wait(barrier, n_tp - 1 + n_ep - 1)
    send_to_all("tp", n_tp, t, lambda p: msg1.at[p], rec1.at[t], ssem.at[0], rsem.at[0])
    send_to_all("tp", n_tp, t, lambda p: extra1.at[p], rec1e.at[t], ssem.at[1], rsem.at[1])

    own_row = (iota((rows, 64), 0) == t).astype(F32)
    rope_raw = jnp.sum(rope_all * own_row, axis=0, keepdims=True)
    cos = trig_v[0:1, 0:64]
    sin = trig_v[1:2, 0:64]
    swap64 = (lax.rem(iota((64, 64), 0) + 32, 64) == iota((64, 64), 1)).astype(F32).astype(BF16)

    def rotated(v):
        return v * cos + dot(v.astype(BF16), swap64) * sin

    rope8 = jnp.broadcast_to(rope_raw, (8, 64))
    new_rope = rotated(rope8)[0:1].astype(BF16)
    nr_v[...] = new_rope

    own_tok = jnp.sum(jnp.where(iota(tok.shape, 0) == t, tok, 0.0), axis=0, keepdims=True)
    for b in range(nblk):
        rows_v[0, b : b + 1, :] = own_tok[:, b * LANES : (b + 1) * LANES]
        for g in range(1, 4):
            rows_v[g, b : b + 1, :] = gains_v[g : g + 1, b * LANES : (b + 1) * LANES]

    routes = routes_v[...].astype(F32)
    upper = (iota((rows, rows), 0) < iota((rows, rows), 1)).astype(F32)
    experts_i = iota((n_ep, rows), 0).astype(F32)
    hits = [(routes[k : k + 1, :] == experts_i).astype(F32) for k in range(2)]
    before = dot(hits[0] + hits[1], upper)
    spread = (lax.shift_right_logical(iota((rows, rows * sub), 1), 3) == iota((rows, rows * sub), 0)).astype(F32)
    lane_row = iota((rows * sub, rows), 1)
    row_of = lax.shift_right_logical(iota((rows * sub, rows), 0), 3)
    gather_col = (lane_row == row_of).astype(F32)
    slot_rows, slot_cols, weight_cols = [], [], []
    for k in range(2):
        slot = routes[k : k + 1, :] * cap_pad + jnp.sum(hits[k] * before, axis=0, keepdims=True)
        slot_rows.append(dot(jnp.broadcast_to(slot, (8, rows)), spread)[0:1])
        slot_cols.append(jnp.sum(gather_col * slot, axis=1, keepdims=True))
        weight_cols.append(jnp.sum(gather_col * rw_v[k : k + 1, :], axis=1, keepdims=True))

    chunk = cap_pad * sub

    def fill_pick(i, carry):
        m = iota((chunk, rows * sub), 0) + i * chunk
        n = iota((chunk, rows * sub), 1)
        slot_m = lax.shift_right_logical(m, 3).astype(F32)
        same = lax.bitwise_and(m, 7) == lax.bitwise_and(n, 7)
        hit = jnp.where(slot_m == slot_rows[0], 1.0, 0.0) + jnp.where(slot_m == slot_rows[1], 1.0, 0.0)
        pick_v[pl.ds(i * chunk, chunk), :] = jnp.where(same, hit, 0.0).astype(BF16)
        return carry

    lax.fori_loop(0, n_ep, fill_pick, 0)
    for k in range(2):
        m = iota((rows * sub, slots * sub), 0)
        n = iota((rows * sub, slots * sub), 1)
        same = lax.bitwise_and(m, 7) == lax.bitwise_and(n, 7)
        hit = jnp.where(lax.shift_right_logical(n, 3).astype(F32) == slot_cols[k], 1.0, 0.0)
        back_v[k] = jnp.where(same, hit, 0.0).astype(BF16)

    wait_bytes(rec1e.at[pl.ds(0, n_tp - 1)], rsem.at[1])
    wait_bytes(rec1.at[pl.ds(0, n_tp - 1)], rsem.at[0])
    ext = rec1e[...][:, 0, :]
    lat_sel = (lax.shift_right_logical(iota((lat_blk, n_tp), 1), per_row.bit_length() - 1) == iota((lat_blk, n_tp), 0)).astype(F32)
    lat_raw = dot(lat_sel.astype(BF16), ext[:, LANES : 2 * LANES].astype(BF16))
    lat_ms = jnp.sum(jnp.sum(lat_raw * lat_raw, axis=1, keepdims=True), axis=0, keepdims=True) / (lat_blk * LANES)
    new_lat = (lat_raw * lax.rsqrt(lat_ms + EPSILON) * lgain_v[...]).astype(BF16)
    nl_v[...] = new_lat
    new_lat_f = new_lat.astype(F32)
    q_pe = rotated(ext[:, 0:64]).astype(BF16)

    def to_blocks(rec, count):
        scat_v[0 : count * lat_blk, :] = rec[...].astype(F32).reshape(count * lat_blk, LANES)
        return [scat_v[pl.ds(j, count, stride=lat_blk), :] for j in range(lat_blk)]

    q_blocks = to_blocks(rec1, n_tp)
    own = q_blocks[0] * new_lat_f[0:1, :]
    for j in range(1, lat_blk):
        own = own + q_blocks[j] * new_lat_f[j : j + 1, :]
    own_score = jnp.sum(own, axis=1, keepdims=True) + jnp.sum(
        q_pe.astype(F32) * new_rope.astype(F32), axis=1, keepdims=True
    )
    own_score = own_score * score_scale
    q_all = jnp.concatenate(q_blocks, axis=1).astype(BF16)
    copies[7].wait()
    copies[8].wait()
    scores = (dot_nt(q_all, cl_v[...]) + dot(q_pe, cr_v[...])) * score_scale
    visible = iota(scores.shape, 1) < len_s[0]
    row_max = jnp.maximum(jnp.max(jnp.where(visible, scores, -jnp.inf), axis=1, keepdims=True), own_score)
    weights = jnp.where(visible, jnp.exp(scores - row_max), 0.0)
    own_weight = jnp.exp(own_score - row_max)
    denominator = jnp.sum(weights, axis=1, keepdims=True) + own_weight
    probs = (weights / denominator).astype(BF16)
    own_prob = (own_weight / denominator).astype(BF16).astype(F32)
    attended = dot(probs, cl_v[...])
    for j in range(lat_blk):
        scat_v[j * n_tp : (j + 1) * n_tp, :] = (
            attended[:, j * LANES : (j + 1) * LANES] + own_prob * new_lat_f[j : j + 1, :]
        )
    for r in range(n_tp):
        msg2[r] = scat_v[pl.ds(r, lat_blk, stride=n_tp), :].astype(BF16)
    rec2[t] = msg2[t]
    send_to_all("tp", n_tp, t, lambda p: msg2.at[p], rec2.at[t], ssem.at[2], rsem.at[2])
    copies[9].wait()
    copies[10].wait()
    wait_bytes(rec2.at[pl.ds(0, n_tp - 1)], rsem.at[2])

    head_lat = jnp.concatenate(to_blocks(rec2, rows), axis=1).astype(BF16)
    values = dot(head_lat, wvu_v[...]).astype(BF16)
    for b in range(nblk):
        scat_v[b * rows : (b + 1) * rows, :] = dot(values, wo_v[:, b * LANES : (b + 1) * LANES])
    for r in range(rows):
        msg3[r] = scat_v[pl.ds(r, nblk, stride=rows), :].astype(BF16)
    rec3[t] = msg3[t]
    send_to_all("tp", n_tp, t, lambda p: msg3.at[p], rec3.at[t], ssem.at[3], rsem.at[3])
    wait_bytes(rec3.at[pl.ds(0, n_tp - 1)], rsem.at[3])

    mixed = rec3[0].astype(F32)
    for r in range(1, n_tp):
        mixed = mixed + rec3[r].astype(F32)

    def block_scale(v):
        total = jnp.sum(jnp.sum(v * v, axis=1, keepdims=True), axis=0, keepdims=True)
        return v * lax.rsqrt(total / (nblk * LANES) + EPSILON)

    resid = (rows_v[0] + block_scale(mixed) * rows_v[1]).astype(BF16).astype(F32)
    expert_in = (block_scale(resid) * rows_v[2]).astype(BF16)
    for c in range(X_SIZE):
        msg4[c] = expert_in[c * sub : (c + 1) * sub, :]
    rec4[t] = msg4[x]
    send_to_all("tp", n_tp, t, lambda p: msg4.at[lax.rem(p, X_SIZE)], rec4.at[t], ssem.at[4], rsem.at[4])
    wait_bytes(rec4.at[pl.ds(0, n_tp - 1)], rsem.at[4])

    own_cols = rec4[...].astype(F32).reshape(rows * sub, LANES).astype(BF16)
    msg5[...] = dot(pick_v[...], own_cols).astype(BF16).reshape(n_ep, chunk, LANES)
    rec5[e] = msg5[e]
    send_to_all("ep", n_ep, e, lambda p: msg5.at[p], rec5.at[e], ssem.at[5], rsem.at[5])
    packed = chunks6.shape[1]
    sel_slot = iota((packed, slots), 1)
    sel_group = jnp.floor((sel_slot.astype(F32) + 0.5) * (1.0 / cap_pad))
    sel_in = sel_slot.astype(F32) - cap_pad * sel_group
    sel_row = iota((packed, slots), 0).astype(F32)
    select = jnp.where((sel_row == sel_group * cap + sel_in) & (sel_in < cap), 1.0, 0.0).astype(BF16)
    exp_slot = iota((slots, packed), 0).astype(F32)
    exp_group = jnp.floor((exp_slot + 0.5) * (1.0 / cap_pad))
    exp_in = exp_slot - cap_pad * exp_group
    exp_row = iota((slots, packed), 1).astype(F32)
    expand = jnp.where((exp_row == exp_group * cap + exp_in) & (exp_in < cap), 1.0, 0.0).astype(BF16)
    wait_bytes(rec5.at[pl.ds(0, n_ep - 1)], rsem.at[5])

    scat_v[0 : slots * sub, :] = rec5[...].astype(F32).reshape(slots * sub, LANES)
    for j in range(sub):
        block = scat_v[pl.ds(j, slots, stride=sub), :].astype(BF16)
        chunks6[x, :, j * LANES : (j + 1) * LANES] = dot(select, block).astype(BF16)

    def x_copy(i, source, target, ss, rs):
        return pltpu.make_async_remote_copy(
            src_ref=source,
            dst_ref=target,
            send_sem=ss,
            recv_sem=rs,
            device_id={"tp": y0 + lax.rem(x + i, X_SIZE)},
            device_id_type=pl.DeviceIdType.MESH,
        )

    for i in range(1, X_SIZE):
        x_copy(i, chunks6.at[x], chunks6.at[x], ssem.at[6 + i], rsem6.at[i]).start()
    copies[11].wait()
    copies[12].wait()
    width = sub * LANES

    def project(c):
        return dot_nt(chunks6[c], wgu_v[:, pl.ds(pl.multiple_of(c * width, width), width)])

    sums = project(x)
    for i in (1, 3, 2):
        c = lax.rem(x + X_SIZE - i, X_SIZE)
        wait_bytes(chunks6.at[c], rsem6.at[i])
        sums = sums + project(c)
    gate = sums[:, 0:64]
    hidden = (gate / (1.0 + jnp.exp(-gate)) * sums[:, 64:128]).astype(BF16)
    copies[13].wait()

    def partial(c):
        return dot(hidden, wd_v[:, pl.ds(pl.multiple_of(c * width, width), width)]).astype(BF16)

    for i in (2, 1, 3):
        c = lax.rem(x + i, X_SIZE)
        msg7[i] = partial(c)
        x_copy(i, msg7.at[i], rec7.at[i], ssem.at[9 + i], rsem7.at[i]).start()
    summed = partial(x).astype(F32)
    for i in (1, 3, 2):
        wait_bytes(rec7.at[i], rsem7.at[i])
        summed = summed + rec7[i].astype(F32)
    summed = summed.astype(BF16)
    for j in range(sub):
        scat_v[pl.ds(j, slots, stride=sub), :] = dot(expand, summed[:, j * LANES : (j + 1) * LANES])
    msg8[...] = scat_v[0 : slots * sub, :].astype(BF16).reshape(n_ep, chunk, LANES)
    rec8[e] = msg8[e]
    send_to_all("ep", n_ep, e, lambda p: msg8.at[p], rec8.at[e], ssem.at[13], rsem.at[6])
    wait_bytes(rec8.at[pl.ds(0, n_ep - 1)], rsem.at[6])

    back = rec8[...].reshape(slots * sub, LANES)
    routed = weight_cols[0] * dot(back_v[0], back) + weight_cols[1] * dot(back_v[1], back)
    msg9[...] = routed.reshape(rows, sub, LANES).astype(BF16)
    rec9[t] = msg9[t]
    send_to_all("tp", n_tp, t, lambda p: msg9.at[p], rec9.at[t], ssem.at[14], rsem.at[7])
    wait_bytes(rec9.at[pl.ds(0, n_tp - 1)], rsem.at[7])
    parts = []
    for c in range(X_SIZE):
        part = rec9[c].astype(F32)
        for r in range(c + X_SIZE, n_tp, X_SIZE):
            part = part + rec9[r].astype(F32)
        parts.append(part)
    total = jnp.concatenate(parts, axis=0)
    out_v[...] = (resid + block_scale(total) * rows_v[3]).astype(BF16)

    wait_bytes(msg1.at[pl.ds(0, n_tp - 1)], ssem.at[0])
    wait_bytes(extra1.at[pl.ds(0, n_tp - 1)], ssem.at[1])
    wait_bytes(msg2.at[pl.ds(0, n_tp - 1)], ssem.at[2])
    wait_bytes(msg3.at[pl.ds(0, n_tp - 1)], ssem.at[3])
    wait_bytes(rec4.at[pl.ds(0, n_tp - 1)], ssem.at[4])
    wait_bytes(msg5.at[pl.ds(0, n_ep - 1)], ssem.at[5])
    for i in range(1, X_SIZE):
        wait_bytes(chunks6.at[x], ssem.at[6 + i])
        wait_bytes(msg7.at[i], ssem.at[9 + i])
    wait_bytes(msg8.at[pl.ds(0, n_ep - 1)], ssem.at[13])
    wait_bytes(msg9.at[pl.ds(0, n_tp - 1)], ssem.at[14])


def on_device(
    tokens,
    norm_gains,
    w_query,
    w_query_rope,
    w_key_up,
    w_value_up,
    w_output,
    w_latent_down,
    latent_gain,
    w_rope_down,
    cache_latent,
    cache_rope,
    lengths,
    routes,
    route_weights,
    w_gate,
    w_up,
    w_down,
):
    n_ep = lax.axis_size("ep")
    n_tp = lax.axis_size("tp")
    rows, width = tokens.shape
    nblk = width // LANES
    sub = nblk // X_SIZE
    cap = min(CAP, rows) if rows == 32 else rows
    cap_pad = CAP_PAD if rows == 32 else rows
    slots = n_ep * cap_pad
    packed = -(-n_ep * cap // 16) * 16
    cache = cache_latent.shape[1]
    latent = cache_latent.shape[2]
    nope_width = w_key_up.shape[1]
    rope_width = w_rope_down.shape[1]
    half = rope_width // 2
    frequency = ROTARY_BASE ** (-jnp.arange(half, dtype=F32) / half)
    angles = lengths.astype(F32)[:, None] * frequency
    cos, sin = jnp.cos(angles), jnp.sin(angles)
    trig = jnp.concatenate(
        [jnp.concatenate([cos, cos], axis=1), jnp.concatenate([-sin, sin], axis=1)], axis=0
    )
    swap = functools.partial(jnp.swapaxes, axis1=-1, axis2=-2)
    operands = (
        tokens,
        norm_gains,
        w_query,
        swap(w_query_rope),
        w_key_up,
        w_value_up,
        w_output,
        swap(w_latent_down),
        latent_gain.reshape(latent // LANES, LANES),
        swap(w_rope_down),
        cache_latent,
        swap(cache_rope),
        lengths,
        swap(routes),
        swap(route_weights),
        swap(w_gate),
        swap(w_up),
        w_down,
        trig,
    )
    in_hbm = pl.BlockSpec(memory_space=pl.ANY)
    in_vmem = pl.BlockSpec(memory_space=pltpu.VMEM)
    in_smem = pl.BlockSpec(memory_space=pltpu.SMEM)
    specs = [in_hbm] * len(operands)
    for i in (8, 13, 14, 18):
        specs[i] = in_vmem
    specs[12] = in_smem
    vm = pltpu.VMEM
    chunk = cap_pad * sub
    scratch = [
        vm((rows, width), BF16),
        vm((4, width), F32),
        vm(w_query.shape, BF16),
        vm((2 * rope_width + latent // n_tp, width), BF16),
        vm(w_key_up.shape[1:], BF16),
        vm(w_value_up.shape[1:], BF16),
        vm(w_output.shape, BF16),
        vm((cache, latent), BF16),
        vm((rope_width, cache), BF16),
        vm((128, width), BF16),
        vm(w_down.shape[1:], BF16),
        pltpu.SemaphoreType.DMA((14,)),
        vm((rows, width), BF16),
        vm((4, nblk, LANES), F32),
        vm((max(nblk * rows, slots * sub), LANES), F32),
        vm((n_tp, 1, 2 * LANES), F32),
        vm((n_tp, 8, LANES), BF16),
        vm((n_tp, 1, 2 * LANES), F32),
        vm((n_tp, 8, LANES), BF16),
        vm((n_tp, 8, LANES), BF16),
        vm((n_tp, 8, LANES), BF16),
        vm((n_tp, nblk, LANES), BF16),
        vm((n_tp, nblk, LANES), BF16),
        vm((X_SIZE, sub, LANES), BF16),
        vm((n_tp, sub, LANES), BF16),
        vm((n_ep, chunk, LANES), BF16),
        vm((n_ep, chunk, LANES), BF16),
        vm((X_SIZE, packed, sub * LANES), BF16),
        vm((X_SIZE, packed, sub * LANES), BF16),
        vm((X_SIZE, packed, sub * LANES), BF16),
        vm((n_ep, chunk, LANES), BF16),
        vm((n_ep, chunk, LANES), BF16),
        vm((n_tp, sub, LANES), BF16),
        vm((n_tp, sub, LANES), BF16),
        vm((slots * sub, rows * sub), BF16),
        vm((2, rows * sub, slots * sub), BF16),
        pltpu.SemaphoreType.DMA((15,)),
        pltpu.SemaphoreType.DMA((8,)),
        pltpu.SemaphoreType.DMA((X_SIZE,)),
        pltpu.SemaphoreType.DMA((X_SIZE,)),
    ]
    kernel = functools.partial(
        step_kernel, n_ep, n_tp, cap, cap_pad, (nope_width + rope_width) ** (-0.5)
    )
    hidden, new_latent, new_rope = pl.pallas_call(
        kernel,
        out_shape=(
            jax.ShapeDtypeStruct((nblk, LANES), BF16),
            jax.ShapeDtypeStruct((latent // LANES, LANES), BF16),
            jax.ShapeDtypeStruct((1, rope_width), BF16),
        ),
        in_specs=specs,
        out_specs=(in_vmem, in_vmem, in_vmem),
        scratch_shapes=scratch,
        compiler_params=pltpu.CompilerParams(
            collective_id=0, has_side_effects=True, vmem_limit_bytes=56 << 20
        ),
    )(*operands)
    return hidden.reshape(1, width), new_latent.reshape(1, latent), new_rope


def solution(mesh):
    in_specs = (
        P("ep", None),
        P(),
        P(None, "tp"),
        P(None, "tp"),
        P("tp", None, None),
        P("tp", None, None),
        P("tp", None),
        P(None, "tp"),
        P(),
        P(),
        P(("ep", "tp"), None, None),
        P(("ep", "tp"), None, None),
        P(("ep", "tp")),
        P("ep", None),
        P("ep", None),
        P("ep", None, "tp"),
        P("ep", None, "tp"),
        P("ep", "tp", None),
    )
    out_specs = (P(("ep", "tp"), None), P(("ep", "tp"), None), P(("ep", "tp"), None))
    return jax.shard_map(
        on_device, mesh=mesh, in_specs=in_specs, out_specs=out_specs, check_vma=False
    )
```
